32 devices in a mesh: ep: 8 (over z, x), tp: 4 (over y, core).
Axes of the slice: x: 2, y: 2, z: 4, core: 2. Of those that a mesh axis runs over, the one named last changes fastest.
Arguments:
- recurrence_query: bfloat16 [1024, 1024], P('ep', 'tp'), may hold values from -6 to 6
- forget_preactivation: bfloat16 [1024, 1024], P('ep', 'tp'), may hold values from -7 to 7
- recurrence_value: bfloat16 [1024, 1024], P('ep', 'tp'), may hold values from -6 to 6
- output_gate_preactivation: bfloat16 [1024, 1024], P('ep', 'tp'), may hold values from -6 to 6
- forget_margin: float32 [1024], P('tp'), may hold values from 0 to 0.1
- surge_log_decay: float32 [8, 1024], P('tp', 'ep'), may hold values from -1.4 to 0
- head_norm_gain: float32 [1024], P('tp'), may hold values from 0.1 to 1.9
- recurrence_output_matrix: bfloat16 [1024, 4096], P('tp'), may hold values from -0.1875 to 0.1875
- second_micro_input: bfloat16 [1024, 4096], P(('ep', 'tp')), may hold values from -6 to 6
- expert_norm_gain: float32 [4096], replicated, may hold values from 0.1 to 1.9
- routes: int32 [1024, 2], P('ep'), may hold values from 0 to 7, all different within a row; in each aligned block of 32 rows (0 to 31, 32 to 63, ...) at most 16 rows name the same one
- router_chosen_logits: float32 [1024, 2], P(('ep', 'tp')), may hold values from -6 to 6
- expert_gate_matrix: bfloat16 [8, 4096, 1408], P('ep', None, 'tp'), may hold values from -0.09375 to 0.09375
- expert_up_matrix: bfloat16 [8, 4096, 1408], P('ep', None, 'tp'), may hold values from -0.09375 to 0.09375
- expert_down_matrix: bfloat16 [8, 1408, 4096], P('ep', 'tp'), may hold values from -0.15625 to 0.15625
Outputs:
- mixed: bfloat16 [1024, 4096], P(('ep', 'tp'))
- moe_out: bfloat16 [1024, 4096], P(('ep', 'tp'))
The draws below stay inside these ranges and needn't reach their ends.
Inputs may be any that keep to these rules, and one draw needn't show every extreme that they name: `routes`: in the rows of one device (aligned blocks of 32 rows) no expert is named more than 16 times, and the experts of a row differ.
All inputs are finite; a program needn't handle non-finite values.
Results may differ from the reference program's by a relative error of at most 0.019.
Values may be sent and summed in bfloat16 or wider, within the bound.
No kernel may reach another device: no remote copies, remote signals or barrier semaphores. Data moves between devices by JAX's collectives and lax.ppermute only.
A program may use at most 128 MiB of HBM per device.

```python
import math
import jax
import jax.numpy as jnp
import numpy as np
from jax import lax

D = 4096
HEADS = 8
KEY = 128
VAL = 128
FF = 1408
TOP = 2
SPAN = 64
SEQ_DEV = 128
TB_DEV = 32
EXPERTS = 8
CAP = 16
TOKENS_A = 1024
TOKENS_B = 1024
N_EP = 8
N_TP = 4


def draw_forget_preactivation(key, part):
    noise_key, shift_key = jax.random.split(jax.random.fold_in(key, 11))
    blocks = TOKENS_A // SEQ_DEV
    shifts = jax.random.uniform(shift_key, (blocks, 1, HEADS * KEY), jnp.float32, -1.0, 1.0)
    noise = jnp.clip(jax.random.normal(noise_key, (blocks, SEQ_DEV, HEADS * KEY), jnp.float32), -6.0, 6.0)
    return (noise + shifts).reshape(TOKENS_A, HEADS * KEY).astype(jnp.bfloat16)


def draw_forget_margin(key, part):
    pick_key, fast_key, slow_key = jax.random.split(jax.random.fold_in(key, 23), 3)
    share = 0.5
    fast_head = jax.random.uniform(pick_key, (HEADS, 1), jnp.float32) < share
    fast_gap = jnp.exp(jax.random.uniform(fast_key, (HEADS, KEY), jnp.float32, math.log(0.04), math.log(0.1)))
    slow_gap = jnp.exp(jax.random.uniform(slow_key, (HEADS, KEY), jnp.float32, math.log(0.3), math.log(1.5))) / TOKENS_A
    return jnp.where(fast_head, fast_gap, slow_gap).reshape(HEADS * KEY).astype(jnp.float32)


def draw_surge_log_decay(key, part):
    spot_key, depth_key = jax.random.split(jax.random.fold_in(key, 37))
    spots = jax.random.randint(spot_key, (HEADS, 2, 1), 0, TOKENS_A)
    depth = jax.random.uniform(depth_key, (HEADS, 2, 1), jnp.float32, math.log(0.5), math.log(0.8))
    hits = spots == jnp.arange(TOKENS_A, dtype=jnp.int32)[None, None, :]
    return jnp.sum(jnp.where(hits, depth, 0.0), axis=1).astype(jnp.float32)


def block_levels(stream_key, extent, shards, low, high):
    level, own = 1.0, jax.random.fold_in(stream_key, 6)
    for axis_at, parts in shards:
        heights = jnp.exp(jax.random.uniform(jax.random.fold_in(own, axis_at), (parts,), jnp.float32, low / len(shards), high / len(shards)))
        level = level * jnp.repeat(heights, extent[axis_at] // parts).reshape([-1 if axis == axis_at else 1 for axis in range(len(extent))])
    return level


def deal_out(own_key, own, number, rows, amount, top, most, slope):
    order = jax.random.permutation(own_key, amount)
    heavy_load, ordinary = shares(amount, rows * top, most, slope, True), shares(amount, rows * top, most, slope, False)
    places = jnp.arange(amount)

    def named(tallies, turn):
        used = int((tallies > 0).sum())
        fixed = max(1, used // 4)
        passed = fixed + (places - fixed + turn * (used - fixed)) % max(1, amount - fixed)
        return jnp.zeros((amount,), jnp.int32).at[order[jnp.where(places < fixed, places, passed)]].set(jnp.asarray(tallies, jnp.int32))

    tallies = jnp.where(number % 4 == 0, named(heavy_load, number // 4), named(ordinary, number - number // 4 - 1))
    mixed = jax.random.permutation(jax.random.fold_in(own, 3), amount)
    donor, taker = mixed[0:amount // 2 * 2:2], mixed[1:amount // 2 * 2:2]
    margin = jnp.minimum(tallies[donor] - 1, most - tallies[taker]) // 2
    margin = jnp.where((donor == order[0]) | (taker == order[0]) | (tallies[taker] == 0), 0, jnp.maximum(margin, 0))
    passed = jax.random.randint(jax.random.fold_in(own, 4), (amount // 2,), 0, 1 << 20) % (margin + 1)
    tallies = tallies.at[donor].add(-passed).at[taker].add(passed)
    items = jnp.searchsorted(jnp.cumsum(tallies), jnp.arange(rows * top), side="right").astype(jnp.int32)
    grid = items.reshape(top, rows).T
    grid = grid[jax.random.permutation(jax.random.fold_in(own, 1), rows)]
    turn = jax.random.randint(jax.random.fold_in(own, 2), (rows, 1), 0, top)
    return jnp.take_along_axis(grid, (jnp.arange(top)[None, :] + turn) % top, axis=1)


def shares(count, total, bound, slope, full):
    weights = [(1 << 20) // math.isqrt(grade ** slope) + 1 for grade in range(1, count + 1)]
    largest = bound if full else min(bound, max(-(-total // count), total * weights[0] // sum(weights)))
    least = 1 if total - largest >= count - 1 else 0
    holding, surplus = [largest] + [least] * (count - 1), total - largest - least * (count - 1)
    while surplus > 0:
        candidates = [i for i in range(1, count) if holding[i] < largest] or [i for i in range(1, count) if holding[i] < bound]
        whole, remaining = sum([weights[i] for i in candidates]), surplus
        for i in candidates:
            addition = min(bound - holding[i], max(1, remaining * weights[i] // whole), surplus)
            holding[i] = holding[i] + addition
            surplus = surplus - addition
    return np.array(holding)


def normal_values(rng, dims, deviation, reach, shards=(), kind=jnp.bfloat16):
    values = jax.random.normal(rng, dims, jnp.float32) * deviation
    if len(shards) > 0:
        values = block_levels(rng, dims, shards, -0.22, 0.18) * values
    return jnp.clip(values, min=-reach, max=reach).astype(kind)


def setup_inputs(seed: int = 0) -> dict:
    streams_of = jax.random.split(jax.random.key(seed), 16)
    recurrence_query = normal_values(streams_of[0], (TOKENS_A, HEADS * KEY), 1.0, 6.0, ((0, 8), (1, 4)))
    forget_preactivation = draw_forget_preactivation(jax.random.fold_in(streams_of[15], 71), 0)
    recurrence_value = normal_values(streams_of[2], (TOKENS_A, HEADS * VAL), 1.0, 6.0, ((0, 8), (1, 4)))
    output_gate_preactivation = normal_values(streams_of[3], (TOKENS_A, HEADS * VAL), 1.0, 6.0, ((0, 8), (1, 4)))
    forget_margin = draw_forget_margin(jax.random.fold_in(streams_of[15], 71), 0)
    surge_log_decay = draw_surge_log_decay(jax.random.fold_in(streams_of[15], 71), 0)
    head_norm_gain = jnp.clip(1.0 + 0.18 * jax.random.normal(streams_of[6], (HEADS * VAL,), jnp.float32), 0.1, 1.9)
    recurrence_output_matrix = normal_values(streams_of[7], (HEADS * VAL, D), (HEADS * VAL) ** -0.5, 0.1875, ((0, 4),))
    second_micro_input = normal_values(streams_of[8], (TOKENS_B, D), 1.0, 6.0, ((0, 32),))
    expert_norm_gain = jnp.clip(1.0 + 0.18 * jax.random.normal(streams_of[9], (D,), jnp.float32), 0.1, 1.9)
    routes_keys = jax.random.split(jax.random.fold_in(streams_of[10], 1), TOKENS_B // TB_DEV)
    routes_turns = jax.random.permutation(jax.random.fold_in(streams_of[10], 3), TOKENS_B // TB_DEV)
    routes = jax.vmap(lambda own, number: deal_out(jax.random.fold_in(streams_of[10], 2), own, number, TB_DEV, EXPERTS, TOP, CAP, 1))(routes_keys, routes_turns).reshape((TOKENS_B, TOP))
    router_chosen_logits = normal_values(streams_of[11], (TOKENS_B, TOP), 1.0, 6.0, ((0, 32),), jnp.float32)
    expert_gate_matrix = normal_values(streams_of[12], (EXPERTS, D, FF), D ** -0.5, 0.09375, ((0, 8), (2, 4)))
    expert_up_matrix = normal_values(streams_of[13], (EXPERTS, D, FF), D ** -0.5, 0.09375, ((0, 8), (2, 4)))
    expert_down_matrix = normal_values(streams_of[14], (EXPERTS, FF, D), FF ** -0.5, 0.15625, ((0, 8), (1, 4)))
    return {"recurrence_query": recurrence_query, "forget_preactivation": forget_preactivation, "recurrence_value": recurrence_value, "output_gate_preactivation": output_gate_preactivation, "forget_margin": forget_margin, "surge_log_decay": surge_log_decay, "head_norm_gain": head_norm_gain, "recurrence_output_matrix": recurrence_output_matrix, "second_micro_input": second_micro_input, "expert_norm_gain": expert_norm_gain, "routes": routes, "router_chosen_logits": router_chosen_logits, "expert_gate_matrix": expert_gate_matrix, "expert_up_matrix": expert_up_matrix, "expert_down_matrix": expert_down_matrix}


epsilon = 1e-06
highest = lax.Precision.HIGHEST

def span_recurrence(query, inflow, decay_logarithm, values):
    number_of_heads, seq_len, key_width = query.shape
    span_count = seq_len // SPAN

    def to_spans(array):
        return array.reshape(number_of_heads, span_count, SPAN, array.shape[-1]).transpose(1, 0, 2, 3)
    lower_mask = jnp.tril(jnp.ones((SPAN, SPAN), bool))

    def advance(carried, inputs):
        query_span, inflow_span, decay_span, value_span = inputs
        running = jnp.cumsum(decay_span, axis=1)
        lifted_query = query_span * jnp.exp(running)
        lowered_inflow = inflow_span * jnp.exp(-running)
        scores = jnp.einsum('htd,hsd->hts', lifted_query, lowered_inflow, precision=highest)
        scores = jnp.where(lower_mask[None, :, :], scores, 0.0)
        output = jnp.einsum('hts,hsv->htv', scores, value_span, precision=highest)
        output = output + jnp.einsum('htd,hdv->htv', lifted_query, carried, precision=highest)
        closing = running[:, -1:, :]
        updated = jnp.exp(closing[:, 0, :])[:, :, None] * carried + jnp.einsum('hsd,hsv->hdv', inflow_span * jnp.exp(closing - running), value_span, precision=highest)
        return (updated, output)
    start_state = jnp.zeros((number_of_heads, key_width, values.shape[-1]), jnp.float32)
    final_state, outputs = lax.scan(advance, start_state, (to_spans(query), to_spans(inflow), to_spans(decay_logarithm), to_spans(values)))
    return (final_state, outputs.transpose(1, 0, 2, 3).reshape(number_of_heads, seq_len, values.shape[-1]))

def split_sum(left, right, groups):
    group_width = left.shape[1] // groups
    total = jnp.zeros((left.shape[0], right.shape[1]), jnp.float32)
    for portion in range(groups):
        piece = jnp.dot(left[:, portion * group_width:(portion + 1) * group_width], right[portion * group_width:(portion + 1) * group_width], preferred_element_type=jnp.float32)
        rounded = lax.optimization_barrier(piece.astype(jnp.bfloat16))
        total = total + rounded.astype(jnp.float32)
    return total.astype(jnp.bfloat16)

def reference(recurrence_query, forget_preactivation, recurrence_value, output_gate_preactivation, forget_margin, surge_log_decay, head_norm_gain, recurrence_output_matrix, second_micro_input, expert_norm_gain, routes, router_chosen_logits, expert_gate_matrix, expert_up_matrix, expert_down_matrix):
    seq_len = recurrence_query.shape[0]

    def heads_leading(array):
        return array.astype(jnp.float32).reshape(seq_len, HEADS, -1).transpose(1, 0, 2)
    closed_flag = jax.nn.sigmoid(-forget_preactivation.astype(jnp.float32)) * forget_margin
    decay_logarithm = heads_leading(jnp.log1p(-closed_flag)) + surge_log_decay[:, :, None]
    query = heads_leading(recurrence_query)
    _, output = span_recurrence(query, heads_leading(closed_flag), decay_logarithm, heads_leading(recurrence_value))
    output = output * lax.rsqrt(lax.optimization_barrier(jnp.mean(output * output, axis=-1, keepdims=True)) + epsilon)
    output = output.transpose(1, 0, 2).reshape(seq_len, -1)
    hidden_a = (output * head_norm_gain * jax.nn.silu(output_gate_preactivation.astype(jnp.float32))).astype(jnp.bfloat16)
    mixed = split_sum(hidden_a, recurrence_output_matrix, N_TP)
    moe_rows = second_micro_input.astype(jnp.float32)
    normed = (moe_rows * lax.rsqrt(lax.optimization_barrier(jnp.mean(moe_rows * moe_rows, axis=-1, keepdims=True)) + epsilon) * expert_norm_gain).astype(jnp.bfloat16)
    flat_routes = routes.reshape(-1)
    copies = flat_routes.shape[0]
    max_rows = N_EP * N_TP * CAP

    def per_expert(written, expert_id):
        picked_order = jnp.argsort((flat_routes != expert_id).astype(jnp.int32), stable=True)[:max_rows]
        picked_order = picked_order.astype(jnp.int32)
        is_live = flat_routes[picked_order] == expert_id
        picked = normed[picked_order // TOP]
        gate_proj = jnp.dot(picked, expert_gate_matrix[expert_id], preferred_element_type=jnp.float32)
        up_proj = jnp.dot(picked, expert_up_matrix[expert_id], preferred_element_type=jnp.float32)
        hidden_b = (jax.nn.silu(gate_proj) * up_proj).astype(jnp.bfloat16)
        result = split_sum(hidden_b, expert_down_matrix[expert_id], N_TP)
        kept_rows = jnp.where(is_live[:, None], result, written[picked_order])
        return (written.at[picked_order].set(kept_rows), None)
    outputs, _ = lax.scan(per_expert, jnp.zeros((copies, D), jnp.bfloat16), jnp.arange(EXPERTS, dtype=jnp.int32))
    route_weight = jax.nn.softmax(router_chosen_logits.astype(jnp.float32), axis=-1)
    moe_out = lax.optimization_barrier(jnp.sum(route_weight[:, :, None] * outputs.reshape(-1, TOP, D).astype(jnp.float32), axis=1))
    return (mixed, moe_out.astype(jnp.bfloat16))
```

```python
import functools

import jax
import jax.numpy as jnp
from jax import lax
from jax.experimental import pallas as pl
from jax.experimental.pallas import tpu as pltpu
from jax.sharding import PartitionSpec as P

TOP = 2
SPAN = 64
EPS = 1e-06
F32 = jnp.float32
BF16 = jnp.bfloat16
NN = (((1,), (0,)), ((), ()))
NT = (((1,), (1,)), ((), ()))
TN = (((0,), (0,)), ((), ()))


def mm(a, b, dims):
    return lax.dot_general(a, b, dims, preferred_element_type=F32)


def split(a):
    hi = a.astype(BF16)
    return hi, (a - hi.astype(F32)).astype(BF16)


def mm_exact_right(a, b, dims):
    hi, lo = split(a)
    return mm(hi, b, dims) + mm(lo, b, dims)


def mm_exact_left(a, b, dims):
    hi, lo = split(b)
    return mm(a, hi, dims) + mm(a, lo, dims)


def mm_split(a, b, dims):
    ahi, alo = split(a)
    bhi, blo = split(b)
    return mm(ahi, bhi, dims) + (mm(ahi, blo, dims) + mm(alo, bhi, dims))


def vmem():
    return pl.BlockSpec(memory_space=pltpu.VMEM)


def dispatch_kernel(ep_axis, capacity, x_ref, gain_ref, routes_ref, logits_ref, weight_ref, *slot_refs):
    me = lax.axis_index(ep_axis)
    rows = x_ref.shape[0]
    slots = capacity * len(slot_refs)
    lane = lax.broadcasted_iota(jnp.int32, (rows, slots), 1)
    expert = jnp.bitwise_xor(lane // capacity, me)
    place_of_lane = lax.rem(lane, capacity).astype(F32)
    logits = logits_ref[...]
    top = jnp.max(logits, axis=1, keepdims=True)
    weights = jnp.exp(logits - top)
    weights = weights / jnp.sum(weights, axis=1, keepdims=True)
    named = jnp.zeros((rows, slots), F32)
    weighted = jnp.zeros((rows, slots), F32)
    for k in range(logits.shape[1]):
        hit = (routes_ref[:, k : k + 1] == expert).astype(F32)
        named = named + hit
        weighted = weighted + hit * weights[:, k : k + 1]
    earlier = lax.broadcasted_iota(jnp.int32, (rows, rows), 0) > lax.broadcasted_iota(
        jnp.int32, (rows, rows), 1
    )
    before = mm(earlier.astype(BF16), named.astype(BF16), NN)
    chosen = jnp.where(before == place_of_lane, named, 0.0)
    weight_ref[...] = jnp.where(before == place_of_lane, weighted, 0.0)
    x = x_ref[...].astype(F32)
    scale = lax.rsqrt(jnp.mean(x * x, axis=-1, keepdims=True) + EPS)
    normed = (x * scale * gain_ref[...]).astype(BF16)
    picked = mm(chosen.T.astype(BF16), normed, NN).astype(BF16)
    for d, ref in enumerate(slot_refs):
        ref[...] = picked[d * capacity : (d + 1) * capacity]


def dispatch(x, gain, routes, logits, capacity, ep_count):
    rows, width = x.shape
    return pl.pallas_call(
        functools.partial(dispatch_kernel, "ep", capacity),
        out_shape=[jax.ShapeDtypeStruct((rows, capacity * ep_count), F32)]
        + [jax.ShapeDtypeStruct((capacity, width), BF16)] * ep_count,
        in_specs=[vmem()] * 4,
        out_specs=[vmem()] * (1 + ep_count),
        name="dispatch",
    )(x, gain.reshape(1, -1), routes, logits)


def ffn_kernel(in_steps, *refs):
    *x_refs, gate_ref, up_ref, down_ref, own_ref, y_ref, send_ref, gate_acc, up_acc, hidden = refs
    step = pl.program_id(0)
    n = own_ref.shape[0]

    @pl.when(step == 0)
    def _():
        gate_acc[...] = jnp.zeros_like(gate_acc)
        up_acc[...] = jnp.zeros_like(up_acc)

    @pl.when(step < in_steps)
    def _():
        x = jnp.concatenate([ref[...] for ref in x_refs], axis=0)
        gate_acc[...] += mm(x, gate_ref[...], NN)
        up_acc[...] += mm(x, up_ref[...], NN)

    @pl.when(step == in_steps - 1)
    def _():
        hidden[...] = (jax.nn.silu(gate_acc[...]) * up_acc[...]).astype(BF16)

    @pl.when(step >= in_steps)
    def _():
        part = mm(hidden[...], down_ref[...], NN).astype(BF16)
        own_ref[...] = part[:n]
        y_ref[...] = part[n : 2 * n]
        send_ref[...] = part[2 * n :]


def ffn(pieces, gate, up, down):
    n, width = pieces[0].shape
    hidden = gate.shape[1]
    in_steps = out_steps = 4
    in_block, out_block = width // in_steps, width // out_steps
    first = lambda k: jnp.minimum(k, in_steps - 1)
    second = lambda k: jnp.maximum(k - in_steps, 0)
    rows = n * len(pieces)
    return pl.pallas_call(
        functools.partial(ffn_kernel, in_steps),
        grid=(in_steps + out_steps,),
        out_shape=[
            jax.ShapeDtypeStruct((n, width), BF16),
            jax.ShapeDtypeStruct((n, width), BF16),
            jax.ShapeDtypeStruct((rows - 2 * n, width), BF16),
        ],
        in_specs=[pl.BlockSpec((n, in_block), lambda k: (0, first(k)))] * len(pieces)
        + [pl.BlockSpec((in_block, hidden), lambda k: (first(k), 0))] * 2
        + [pl.BlockSpec((hidden, out_block), lambda k: (0, second(k)))],
        out_specs=[
            pl.BlockSpec((n, out_block), lambda k: (0, second(k))),
            pl.BlockSpec((n, out_block), lambda k: (0, second(k))),
            pl.BlockSpec((rows - 2 * n, out_block), lambda k: (0, second(k))),
        ],
        scratch_shapes=[
            pltpu.VMEM((rows, hidden), F32),
            pltpu.VMEM((rows, hidden), F32),
            pltpu.VMEM((rows, hidden), BF16),
        ],
        cost_estimate=pl.CostEstimate(
            flops=6 * rows * width * hidden,
            bytes_accessed=6 * width * hidden + 4 * rows * width,
            transcendentals=rows * hidden,
        ),
        name="experts",
    )(*pieces, gate, up, down)


def local_kernel(heads, q_ref, f_ref, v_ref, margin_ref, surge_ref, pay_ref, lifted_ref, out_ref, state_ref, total_ref):
    rows = q_ref.shape[0]
    key = q_ref.shape[1] // heads
    closed = jax.nn.sigmoid(-f_ref[...].astype(F32)) * margin_ref[...]
    base = jnp.log1p(-closed)
    lower = lax.broadcasted_iota(jnp.int32, (SPAN, SPAN), 0) >= lax.broadcasted_iota(
        jnp.int32, (SPAN, SPAN), 1
    )
    ones = lower.astype(BF16)
    total_ref[...] = jnp.zeros_like(total_ref)
    pay_ref[...] = jnp.zeros_like(pay_ref)
    for h in range(heads):
        cols = slice(h * key, (h + 1) * key)
        decay = base[:, cols] + surge_ref[:, h : h + 1]
        before = jnp.zeros((1, key), F32)
        state = None
        for s in range(rows // SPAN):
            at = slice(s * SPAN, (s + 1) * SPAN)
            part = decay[at]
            p0, p1 = split(part)
            p2 = (part - p0.astype(F32) - p1.astype(F32)).astype(BF16)
            running = mm(ones, p0, NN) + (mm(ones, p1, NN) + mm(ones, p2, NN))
            query = q_ref[at, cols].astype(F32)
            inflow = closed[at, cols]
            value = v_ref[at, cols]
            middle = running[SPAN // 2 : SPAN // 2 + 1]
            closing = running[SPAN - 1 : SPAN]
            scores = mm_split(
                query * jnp.exp(running - middle), inflow * jnp.exp(middle - running), NT
            )
            scores = jnp.where(lower, scores, 0.0)
            out = mm_exact_right(scores, value, NN)
            if state is not None:
                out = out + mm_split(query * jnp.exp(running), state, NT)
            out_ref[at, cols] = out
            lifted_ref[at, cols] = query * jnp.exp(running + before)
            update = mm_exact_left(value, inflow * jnp.exp(closing - running), TN)
            state = update if state is None else jnp.exp(closing) * state + update
            before = before + closing
        state_ref[cols, :] = state
        pay_ref[cols, :] = state.astype(BF16)
        total_ref[h : h + 1, :] = before
        hi, lo = split(before)
        pay_ref[heads * key + h : heads * key + h + 1, :] = hi
        pay_ref[heads * key + heads + h : heads * key + heads + h + 1, :] = lo


def local_recurrence(q, f, v, margin, surge, heads):
    rows, cols = q.shape
    key = cols // heads
    return pl.pallas_call(
        functools.partial(local_kernel, heads),
        out_shape=[
            jax.ShapeDtypeStruct((cols + 16, key), BF16),
            jax.ShapeDtypeStruct((rows, cols), F32),
            jax.ShapeDtypeStruct((rows, cols), F32),
            jax.ShapeDtypeStruct((cols, key), F32),
            jax.ShapeDtypeStruct((8, key), F32),
        ],
        in_specs=[vmem()] * 5,
        out_specs=[vmem()] * 5,
        name="local_recurrence",
    )(q, f, v, margin.reshape(1, -1), surge.T)


def scan_kernel(heads, bit, *refs):
    got_ref, state_ref, total_ref = refs[:3]
    refs = refs[3:]
    pre_ref = pretotal_ref = None
    if bit > 1:
        pre_ref, pretotal_ref = refs[:2]
        refs = refs[2:]
    newpre_ref, newpretotal_ref, *rest = refs
    key = state_ref.shape[1]
    upper = jnp.bitwise_and(lax.axis_index("ep"), bit) != 0
    at = heads * key
    got_total = got_ref[at : at + heads, :].astype(F32) + got_ref[at + heads : at + 2 * heads, :].astype(F32)
    total = total_ref[0:heads, :]
    newpretotal_ref[...] = jnp.zeros_like(newpretotal_ref)
    before = jnp.zeros((heads, key), F32) if pre_ref is None else pretotal_ref[0:heads, :]
    newpretotal_ref[0:heads, :] = jnp.where(upper, before + got_total, before)
    if rest:
        pay_ref, newstate_ref, newtotal_ref = rest
        newtotal_ref[...] = jnp.zeros_like(newtotal_ref)
        joined = total + got_total
        newtotal_ref[0:heads, :] = joined
        pay_ref[...] = jnp.zeros_like(pay_ref)
        hi, lo = split(joined)
        pay_ref[at : at + heads, :] = hi
        pay_ref[at + heads : at + 2 * heads, :] = lo
    for h in range(heads):
        cols = slice(h * key, (h + 1) * key)
        got = got_ref[cols, :].astype(F32)
        if pre_ref is None:
            newpre_ref[cols, :] = jnp.where(upper, got, 0.0)
        else:
            pre = pre_ref[cols, :]
            newpre_ref[cols, :] = jnp.where(upper, jnp.exp(before[h : h + 1]) * got + pre, pre)
        if rest:
            mine = state_ref[cols, :]
            new = jnp.where(
                upper,
                jnp.exp(total[h : h + 1]) * got + mine,
                jnp.exp(got_total[h : h + 1]) * mine + got,
            )
            newstate_ref[cols, :] = new
            pay_ref[cols, :] = new.astype(BF16)


def scan_step(heads, bit, last, got, state, total, pre, pretotal):
    shape = jax.ShapeDtypeStruct
    out = [shape(state.shape, F32), shape(total.shape, F32)]
    if not last:
        out += [shape(got.shape, BF16), shape(state.shape, F32), shape(total.shape, F32)]
    args = [got, state, total] + ([pre, pretotal] if bit > 1 else [])
    return pl.pallas_call(
        functools.partial(scan_kernel, heads, bit),
        out_shape=out,
        in_specs=[vmem()] * len(args),
        out_specs=[vmem()] * len(out),
        name="scan_step",
    )(*args)


def mix_kernel(heads, lifted_ref, local_ref, pre_ref, og_ref, gain_ref, w_ref, own_ref, y_ref, send_ref, plain, hidden):
    step = pl.program_id(0)
    rows = own_ref.shape[0]

    @pl.when(step == 0)
    def _():
        key = pre_ref.shape[1]
        for h in range(heads):
            cols = slice(h * key, (h + 1) * key)
            out = local_ref[:, cols] + mm_split(lifted_ref[:, cols], pre_ref[cols, :], NT)
            out = out * lax.rsqrt(jnp.mean(out * out, axis=-1, keepdims=True) + EPS)
            plain[:, cols] = out * gain_ref[:, cols] * jax.nn.silu(og_ref[:, cols].astype(F32))
        mine = lax.axis_index("tp")
        for j, other in enumerate((0, 2, 1, 3)):
            at = pl.multiple_of(jnp.bitwise_xor(mine, other) * rows, rows)
            hidden[j * rows : (j + 1) * rows, :] = plain[pl.ds(at, rows), :].astype(BF16)

    part = mm(hidden[...], w_ref[...], NN).astype(BF16)
    own_ref[...] = part[:rows]
    y_ref[...] = part[rows : 2 * rows]
    send_ref[...] = part[2 * rows :]


def mix(heads, lifted, local, pre, og, gain, w):
    seq, cols = lifted.shape
    width = w.shape[1]
    rows = seq // 4
    steps = 4
    block = width // steps
    whole = lambda a: pl.BlockSpec(a.shape, lambda k: (0, 0))
    gain = gain.reshape(1, -1)
    return pl.pallas_call(
        functools.partial(mix_kernel, heads),
        grid=(steps,),
        out_shape=[
            jax.ShapeDtypeStruct((rows, width), BF16),
            jax.ShapeDtypeStruct((rows, width), BF16),
            jax.ShapeDtypeStruct((2 * rows, width), BF16),
        ],
        in_specs=[whole(a) for a in (lifted, local, pre, og, gain)]
        + [pl.BlockSpec((cols, block), lambda k: (0, k))],
        out_specs=[
            pl.BlockSpec((rows, block), lambda k: (0, k)),
            pl.BlockSpec((rows, block), lambda k: (0, k)),
            pl.BlockSpec((2 * rows, block), lambda k: (0, k)),
        ],
        scratch_shapes=[pltpu.VMEM((seq, cols), F32), pltpu.VMEM((seq, cols), BF16)],
        cost_estimate=pl.CostEstimate(
            flops=2 * seq * cols * width, bytes_accessed=2 * cols * width + 2 * seq * width, transcendentals=0
        ),
        name="mix",
    )(lifted, local, pre, og, gain, w)


def swap(value, axis, bit):
    size = lax.axis_size(axis)
    return lax.ppermute(value, axis, [(i, i ^ bit) for i in range(size)])


def pair_sum(a, b):
    return (a.astype(F32) + b.astype(F32)).astype(BF16)


def fold(own, y, send):
    n = own.shape[0]
    got = swap(send, "tp", 1)
    y_sum = pair_sum(y, got[n:])
    own_sum = pair_sum(own, got[:n])
    return pair_sum(own_sum, swap(y_sum, "tp", 2))


def exchange_device(
    recurrence_query,
    forget_preactivation,
    recurrence_value,
    output_gate_preactivation,
    forget_margin,
    surge_log_decay,
    head_norm_gain,
    recurrence_output_matrix,
    second_micro_input,
    expert_norm_gain,
    routes,
    router_chosen_logits,
    expert_gate_matrix,
    expert_up_matrix,
    expert_down_matrix,
):
    heads = surge_log_decay.shape[0]
    ep_count = lax.axis_size("ep")
    tok_rows = second_micro_input.shape[0]
    capacity = 2 * tok_rows * TOP // ep_count
    tp_rank = lax.axis_index("tp")
    gate, up, down = (expert_gate_matrix[0], expert_up_matrix[0], expert_down_matrix[0])

    own_routes = lax.dynamic_slice_in_dim(routes, tp_rank * tok_rows, tok_rows, 0)
    weights, *blocks = dispatch(
        second_micro_input, expert_norm_gain, own_routes, router_chosen_logits, capacity, ep_count
    )
    half = ep_count // 2
    near = list(range(half))
    groups = [near] + [[d, d + 1] for d in range(half, ep_count, 2)]
    arrived = {0: blocks[0]}
    for d in range(1, ep_count):
        arrived[d] = swap(blocks[d], "ep", d)

    payload, lifted, local, state, total = local_recurrence(
        recurrence_query,
        forget_preactivation,
        recurrence_value,
        forget_margin,
        surge_log_decay,
        heads,
    )
    pre = pretotal = None
    bit = 1
    while bit < ep_count:
        last = bit * 2 >= ep_count
        got = swap(payload, "ep", bit)
        pre, pretotal, *rest = scan_step(heads, bit, last, got, state, total, pre, pretotal)
        if rest:
            payload, state, total = rest
        bit *= 2
    mixed = fold(
        *mix(
            heads,
            lifted,
            local,
            pre,
            output_gate_preactivation,
            head_norm_gain,
            recurrence_output_matrix,
        )
    )

    moe_out = jnp.zeros((tok_rows, second_micro_input.shape[1]), F32)
    for group in groups:
        own = jnp.concatenate([arrived[d] for d in group], axis=0)
        across = swap(own, "tp", 2)
        pieces = [own, across, swap(own, "tp", 1), swap(across, "tp", 1)]
        summed = fold(*ffn(pieces, gate, up, down))
        back = []
        for at, d in enumerate(group):
            block = summed[at * capacity : (at + 1) * capacity]
            back.append(block if d == 0 else swap(block, "ep", d))
        share = weights[:, group[0] * capacity : (group[-1] + 1) * capacity]
        moe_out = moe_out + jnp.dot(
            share,
            jnp.concatenate(back, axis=0).astype(F32),
            precision=lax.Precision.HIGHEST,
            preferred_element_type=F32,
        )
    return (mixed, moe_out.astype(BF16))


def entering_state(value, axis):
    size, mine = (lax.axis_size(axis), lax.axis_index(axis))
    everything = jax.tree.map(lambda part: lax.all_gather(part.astype(BF16), axis), value)
    start = jax.tree.map(jnp.zeros_like, value)

    def hop(k, before):
        later = jax.tree.map(lambda part: part[k].astype(F32), everything)
        new = (before[0] + later[0], jnp.exp(later[0])[:, :, None] * before[1] + later[1])
        return jax.tree.map(lambda a, b: jnp.where(k < mine, a, b), new, before)

    return lax.fori_loop(0, size, hop, start)


def span_recurrence(query, inflow, decay_logarithm, values):
    highest = lax.Precision.HIGHEST
    number_of_heads, seq_len, key_width = query.shape
    span_count = seq_len // SPAN

    def to_spans(array):
        return array.reshape(number_of_heads, span_count, SPAN, array.shape[-1]).transpose(1, 0, 2, 3)

    lower_mask = jnp.tril(jnp.ones((SPAN, SPAN), bool))

    def advance(carried, inputs):
        query_span, inflow_span, decay_span, value_span = inputs
        running = jnp.cumsum(decay_span, axis=1)
        middle = running[:, SPAN // 2 : SPAN // 2 + 1, :]
        scores = jnp.einsum(
            "htd,hsd->hts",
            query_span * jnp.exp(running - middle),
            inflow_span * jnp.exp(middle - running),
            precision=highest,
        )
        scores = jnp.where(lower_mask[None, :, :], scores, 0.0)
        output = jnp.einsum("hts,hsv->htv", scores, value_span, precision=highest)
        output = output + jnp.einsum(
            "htd,hdv->htv", query_span * jnp.exp(running), carried, precision=highest
        )
        closing = running[:, -1:, :]
        updated = jnp.exp(closing[:, 0, :])[:, :, None] * carried + jnp.einsum(
            "hsd,hsv->hdv", inflow_span * jnp.exp(closing - running), value_span, precision=highest
        )
        return (updated, output)

    start_state = jnp.zeros((number_of_heads, key_width, values.shape[-1]), F32)
    final_state, outputs = lax.scan(
        advance, start_state, (to_spans(query), to_spans(inflow), to_spans(decay_logarithm), to_spans(values))
    )
    return (
        final_state,
        outputs.transpose(1, 0, 2, 3).reshape(number_of_heads, seq_len, values.shape[-1]),
    )


def slot_positions(block_routes, expert_count):
    chosen = block_routes.reshape(-1)
    table = (chosen[:, None] == jnp.arange(expert_count, dtype=jnp.int32)[None, :]).astype(jnp.int32)
    before = jnp.cumsum(table, axis=0) - table
    return (chosen, jnp.sum(before * table, axis=1))


def collective_device(
    recurrence_query,
    forget_preactivation,
    recurrence_value,
    output_gate_preactivation,
    forget_margin,
    surge_log_decay,
    head_norm_gain,
    recurrence_output_matrix,
    second_micro_input,
    expert_norm_gain,
    routes,
    router_chosen_logits,
    expert_gate_matrix,
    expert_up_matrix,
    expert_down_matrix,
):
    number_of_heads = surge_log_decay.shape[0]
    seq_len = recurrence_query.shape[0]

    def heads_leading(array):
        return array.astype(F32).reshape(seq_len, number_of_heads, -1).transpose(1, 0, 2)

    closed = jax.nn.sigmoid(-forget_preactivation.astype(F32)) * forget_margin
    decay = heads_leading(jnp.log1p(-closed)) + surge_log_decay[:, :, None]
    query = heads_leading(recurrence_query)
    final_state, local_out = span_recurrence(
        query, heads_leading(closed), decay, heads_leading(recurrence_value)
    )
    running = jnp.cumsum(decay, axis=1)
    entering = entering_state((running[:, -1, :], final_state), "ep")
    output = local_out + jnp.einsum(
        "htd,hdv->htv", query * jnp.exp(running), entering[1], precision=lax.Precision.HIGHEST
    )
    output = output * lax.rsqrt(jnp.mean(output * output, axis=-1, keepdims=True) + EPS)
    output = output.transpose(1, 0, 2).reshape(seq_len, -1)
    hidden_a = (
        output * head_norm_gain * jax.nn.silu(output_gate_preactivation.astype(F32))
    ).astype(BF16)
    tp_count = lax.axis_size("tp")
    tp_rank = lax.axis_index("tp")
    expert_count = lax.axis_size("ep")
    tok_rows, width = second_micro_input.shape
    capacity = 2 * tok_rows * TOP // expert_count
    moe_rows = second_micro_input.astype(F32)
    normed = (
        moe_rows
        * lax.rsqrt(jnp.mean(moe_rows * moe_rows, axis=-1, keepdims=True) + EPS)
        * expert_norm_gain
    ).astype(BF16)
    own_routes = lax.dynamic_slice_in_dim(routes, tp_rank * tok_rows, tok_rows, 0)
    own_chosen, own_places = slot_positions(own_routes, expert_count)
    copy_source = jnp.arange(tok_rows * TOP, dtype=jnp.int32) // TOP
    buffer = jnp.zeros((expert_count * capacity, width), BF16)
    buffer = buffer.at[own_chosen * capacity + own_places].set(normed[copy_source])
    arrived = lax.all_to_all(buffer, "ep", split_axis=0, concat_axis=0, tiled=True)
    rows = lax.all_gather(arrived, "tp", axis=0, tiled=True)
    gate_proj = jnp.dot(rows, expert_gate_matrix[0], preferred_element_type=F32)
    up_proj = jnp.dot(rows, expert_up_matrix[0], preferred_element_type=F32)
    hidden_b = (jax.nn.silu(gate_proj) * up_proj).astype(BF16)
    mix_rows = seq_len // tp_count
    slots = expert_count * capacity
    hidden_a = hidden_a.reshape(tp_count, mix_rows, -1)
    hidden_b = hidden_b.reshape(tp_count, slots, -1)
    pieces = []
    for block in range(tp_count):
        pieces.append(jnp.dot(hidden_a[block], recurrence_output_matrix, preferred_element_type=F32))
        pieces.append(jnp.dot(hidden_b[block], expert_down_matrix[0], preferred_element_type=F32))
    summed = lax.psum_scatter(
        jnp.concatenate(pieces, axis=0).astype(BF16), "tp", scatter_dimension=0, tiled=True
    )
    mixed = summed[:mix_rows]
    returned = lax.all_to_all(summed[mix_rows:], "ep", split_axis=0, concat_axis=0, tiled=True)
    picked = returned[own_chosen * capacity + own_places]
    route_weight = jax.nn.softmax(router_chosen_logits, axis=-1)
    moe_out = jnp.sum(
        route_weight[:, :, None] * picked.reshape(tok_rows, TOP, width).astype(F32), axis=1
    )
    return (mixed, moe_out.astype(BF16))


def solution(mesh):
    ep_count, tp_count = mesh.shape["ep"], mesh.shape["tp"]
    hypercube = ep_count & (ep_count - 1) == 0 and 4 <= ep_count <= 8 and tp_count == 4
    return jax.shard_map(
        exchange_device if hypercube else collective_device,
        mesh=mesh,
        in_specs=(
            P("ep", "tp"),
            P("ep", "tp"),
            P("ep", "tp"),
            P("ep", "tp"),
            P("tp"),
            P("tp", "ep"),
            P("tp"),
            P("tp", None),
            P(("ep", "tp"), None),
            P(),
            P("ep", None),
            P(("ep", "tp"), None),
            P("ep", None, "tp"),
            P("ep", None, "tp"),
            P("ep", "tp", None),
        ),
        out_specs=(P(("ep", "tp"), None), P(("ep", "tp"), None)),
        check_vma=False,
    )
```
